32 devices in a mesh: sp: 4 (over z), tp: 4 (over y, x), dp: 2 (over core).
Axes of the slice: x: 2, y: 2, z: 4, core: 2. Of those that a mesh axis runs over, the one named last changes fastest.
Arguments:
- latent: bfloat16 [8192, 2048], P(('dp', 'sp', 'tp')), parts along dimension 0, may hold values from -6 to 6
- cond: bfloat16 [4096], P('dp'), parts along dimension 0, may hold values from -6 to 6
- ctx_rows: bfloat16 [2048, 2048], P(('dp', 'sp')), parts along dimension 0, may hold values from -6 to 6
- ctx_cond: bfloat16 [2048], replicated, may hold values from -6 to 6
- mod_weight: bfloat16 [3, 2048, 2048], P(None, 'sp', 'tp'), may hold values from -0.125 to 0.125
- norm_gain: float32 [2048], replicated, may hold values from 0.1 to 1.9
- out_gain: float32 [2048], replicated, may hold values from 0.1 to 1.9
- w_query: bfloat16 [2048, 1024], replicated, may hold values from -16 to 16
- w_key: bfloat16 [2048, 256], replicated, may hold values from -1 to 1
- w_value: bfloat16 [2048, 256], replicated, may hold values from -0.125 to 0.125
- w_out: bfloat16 [1024, 2048], replicated, may hold values from -0.1875 to 0.1875
- sink: float32 [16], replicated, may hold values from 3 to 8
Outputs:
- updated: bfloat16 [8192, 2048], P(('dp', 'sp', 'tp')), parts along dimension 0
The draws below stay inside these ranges and needn't reach their ends.
There are 2 independent parts, one for each index of `dp`. The reference program is written for one: setup_inputs(seed, part) draws one part's arguments, and reference() takes and returns one part's arrays. A program takes and returns all parts, laid end to end along the dimension named above; an argument that names none is the same for every part. Nothing has to cross between parts.
All inputs are finite; a program needn't handle non-finite values.
Results may differ from the reference program's by a relative error of at most 0.0053.
Values may be sent and summed in bfloat16 or wider, within the bound.
A program may use at most 128 MiB of HBM per device.

```python
import jax
import jax.numpy as jnp
from jax import lax

D = 2048
HEADS = 16
KV_HEADS = 4
HEAD_DIM = 64
WINDOW = 128
SPAN = 128
GRID_W = 64
CTX = 1024
SEQ = 4096


def shared_weights(key):
    base_key = jax.random.fold_in(key, 11)
    first_key, second_key = jax.random.split(base_key, 2)
    key_matrix = jax.random.normal(first_key, (D, KV_HEADS * HEAD_DIM), jnp.float32) * D ** (-0.5)
    key_matrix = jnp.clip(key_matrix, -1.0, 1.0)
    query_matrix = jax.random.normal(second_key, (D, HEADS * HEAD_DIM), jnp.float32) * D ** (-0.5)
    return (key_matrix, query_matrix)


def draw_w_key(key, part):
    return shared_weights(key)[0].astype(jnp.bfloat16)


def draw_w_query(key, part):
    key_matrix, query_matrix = shared_weights(key)
    query_matrix = jnp.clip(query_matrix, -16.0, 16.0)
    return query_matrix.astype(jnp.bfloat16)


def levels(own_key, dims, cuts, least, high):
    def one(axis_at, blocks):
        steps = jax.random.uniform(jax.random.fold_in(jax.random.fold_in(own_key, 6), axis_at), (blocks,), jnp.float32, least / len(cuts), high / len(cuts))
        return jnp.repeat(jnp.exp(steps), dims[axis_at] // blocks).reshape((-1,) + (1,) * (len(dims) - axis_at - 1))

    factor_of = one(*cuts[0])
    for cut in cuts[1:]:
        factor_of = factor_of * one(*cut)
    return factor_of


def gaussian(own_key, dims, scale, most, shards=(), kind=jnp.bfloat16):
    level = levels(own_key, dims, shards, -0.22, 0.18) if shards else 1.0
    result = jax.random.normal(own_key, dims, jnp.float32) * scale * level
    return jnp.minimum(jnp.maximum(result, -most), most).astype(kind)


def setup_inputs(seed: int = 0, part: int = 0) -> dict:
    arg_keys = jax.random.split(jax.random.key(seed), 13)
    part_splits = jax.random.split(jax.random.fold_in(arg_keys[12], part), 13)
    return {
        "latent": gaussian(part_splits[0], (SEQ, D), 1.0, 6.0, ((0, 16),)),
        "cond": gaussian(part_splits[1], (D,), 1.0, 6.0),
        "ctx_rows": gaussian(part_splits[2], (CTX, D), 1.0, 6.0, ((0, 4),)),
        "ctx_cond": gaussian(arg_keys[3], (D,), 1.0, 6.0),
        "mod_weight": gaussian(arg_keys[4], (3, D, D), D ** -0.5, 0.125, ((1, 4), (2, 4))),
        "norm_gain": jnp.clip(1.0 + 0.18 * jax.random.normal(arg_keys[5], (D,), jnp.float32), 0.1, 1.9),
        "out_gain": jnp.clip(1.0 + 0.18 * jax.random.normal(arg_keys[6], (D,), jnp.float32), 0.1, 1.9),
        "w_query": draw_w_query(jax.random.fold_in(arg_keys[12], 71), part),
        "w_key": draw_w_key(jax.random.fold_in(arg_keys[12], 71), part),
        "w_value": gaussian(arg_keys[9], (D, KV_HEADS * HEAD_DIM), D ** -0.5, 0.125),
        "w_out": gaussian(arg_keys[10], (HEADS * HEAD_DIM, D), (HEADS * HEAD_DIM) ** -0.5, 0.1875),
        "sink": jnp.clip(jax.random.uniform(arg_keys[11], (HEADS,), jnp.float32, 3.0, 8.0), 3.0, 8.0),
    }


EPSILON = 1e-06
NEG_BIG = -1e+30

def rope_angles(positions, head_width):
    freq_count = head_width // 4
    inverse = 10000.0 ** (-jnp.arange(freq_count, dtype=jnp.float32) / freq_count)
    grid_row = (positions // GRID_W).astype(jnp.float32)
    grid_col = (positions % GRID_W).astype(jnp.float32)
    angles = jnp.concatenate([grid_row[:, None] * inverse, grid_col[:, None] * inverse], axis=-1)
    return (jnp.cos(angles), jnp.sin(angles))

def rotate(values, cosine, sine_table):
    half_width = values.shape[-1] // 2
    floats = values.astype(jnp.float32)
    first = floats[..., :half_width]
    second = floats[..., half_width:]
    cos_b = cosine[:, None]
    sin_b = sine_table[:, None]
    return jnp.concatenate([first * cos_b - second * sin_b, first * sin_b + second * cos_b], axis=-1).astype(jnp.bfloat16)

def mod_norm(rows, gain, scale_vec, shift_vec):
    floats = rows.astype(jnp.float32)
    normed = floats * lax.rsqrt(lax.optimization_barrier(jnp.mean(floats * floats, axis=-1, keepdims=True)) + EPSILON) * gain
    return (normed * (1.0 + scale_vec) + shift_vec).astype(jnp.bfloat16)

def band_attention(query_rot, query_plain, key_padded, value_padded, key_ctx, value_ctx, sink_group, offset, seq_total):
    length_dev, groups, head_width = query_rot.shape
    blocks = length_dev // SPAN
    query_blocks = query_rot.reshape(blocks, SPAN, groups, head_width).astype(jnp.float32)
    plain_blocks = query_plain.reshape(blocks, SPAN, groups, head_width).astype(jnp.float32)
    key_split = key_padded.reshape(blocks + 2, SPAN, head_width)
    value_split = value_padded.reshape(blocks + 2, SPAN, head_width)
    key_band = jnp.concatenate([key_split[:-2], key_split[1:-1], key_split[2:]], axis=1).astype(jnp.float32)
    value_band = jnp.concatenate([value_split[:-2], value_split[1:-1], value_split[2:]], axis=1).astype(jnp.float32)
    factor = head_width ** (-0.5)
    local = jnp.einsum('nigd,njd->ngij', query_blocks, key_band) * factor
    block_start = offset + jnp.arange(blocks, dtype=jnp.int32) * SPAN
    query_pos = block_start[:, None, None] + jnp.arange(SPAN, dtype=jnp.int32)[None, :, None]
    key_pos = block_start[:, None, None] + jnp.arange(3 * SPAN, dtype=jnp.int32)[None, None, :] - SPAN
    allowed = (jnp.abs(query_pos - key_pos) <= WINDOW) & (key_pos >= 0) & (key_pos < seq_total)
    local = jnp.where(allowed[:, None], local, NEG_BIG)
    context = jnp.einsum('nigd,cd->ngic', plain_blocks, key_ctx.astype(jnp.float32)) * factor
    sink_col = sink_group.astype(jnp.float32)[None, :, None]
    row_max = jnp.maximum(jnp.maximum(lax.optimization_barrier(jnp.max(local, axis=-1)), lax.optimization_barrier(jnp.max(context, axis=-1))), sink_col)
    exp_local = jnp.exp(local - row_max[..., None])
    exp_ctx = jnp.exp(context - row_max[..., None])
    exp_sink = jnp.exp(sink_col - row_max)
    denom = lax.optimization_barrier(jnp.sum(exp_local, axis=-1)) + lax.optimization_barrier(jnp.sum(exp_ctx, axis=-1)) + exp_sink
    weight_local = (exp_local / denom[..., None]).astype(jnp.bfloat16)
    weight_ctx = (exp_ctx / denom[..., None]).astype(jnp.bfloat16)
    mixed = jnp.einsum('ngij,njd->nigd', weight_local.astype(jnp.float32), value_band) + jnp.einsum('ngic,cd->nigd', weight_ctx.astype(jnp.float32), value_ctx.astype(jnp.float32))
    return mixed.astype(jnp.bfloat16).reshape(length_dev, groups * head_width)

def reference(latent, cond, ctx_rows, ctx_cond, mod_weight, norm_gain, out_gain, w_query, w_key, w_value, w_out, sink):
    vectors = jax.nn.silu(jnp.stack([cond, ctx_cond]).astype(jnp.float32)).astype(jnp.bfloat16)
    shift_vec = jnp.dot(vectors, mod_weight[0], preferred_element_type=jnp.float32)
    scale_vec = jnp.dot(vectors, mod_weight[1], preferred_element_type=jnp.float32)
    gate_vec = jnp.dot(vectors[:1], mod_weight[2], preferred_element_type=jnp.float32)[0]
    hidden = mod_norm(latent, norm_gain, scale_vec[0], shift_vec[0])
    ctx_hidden = mod_norm(ctx_rows, norm_gain, scale_vec[1], shift_vec[1])
    query = jnp.dot(hidden, w_query, preferred_element_type=jnp.float32).astype(jnp.bfloat16)
    keys = jnp.dot(hidden, w_key, preferred_element_type=jnp.float32).astype(jnp.bfloat16)
    values = jnp.dot(hidden, w_value, preferred_element_type=jnp.float32).astype(jnp.bfloat16)
    ctx_keys = jnp.dot(ctx_hidden, w_key, preferred_element_type=jnp.float32).astype(jnp.bfloat16)
    ctx_values = jnp.dot(ctx_hidden, w_value, preferred_element_type=jnp.float32).astype(jnp.bfloat16)
    seq_total = latent.shape[0]
    groups = HEADS // KV_HEADS
    cosine, sine_table = rope_angles(jnp.arange(seq_total, dtype=jnp.int32), HEAD_DIM)
    query_heads = query.reshape(seq_total, HEADS, HEAD_DIM)
    query_rot = rotate(query_heads, cosine, sine_table).reshape(seq_total, KV_HEADS, groups, HEAD_DIM)
    query_grid = query_heads.reshape(seq_total, KV_HEADS, groups, HEAD_DIM)
    key_rot = rotate(keys.reshape(seq_total, KV_HEADS, HEAD_DIM), cosine, sine_table)
    value_grid = values.reshape(seq_total, KV_HEADS, HEAD_DIM)
    padding = jnp.zeros((SPAN, KV_HEADS, HEAD_DIM), jnp.bfloat16)
    key_pad = jnp.concatenate([padding, key_rot, padding], axis=0)
    value_pad = jnp.concatenate([padding, value_grid, padding], axis=0)

    def one_head(operands):
        return band_attention(operands[0], operands[1], operands[2], operands[3], operands[4], operands[5], operands[6], 0, seq_total)
    stacked = lax.map(one_head, (jnp.transpose(query_rot, (1, 0, 2, 3)), jnp.transpose(query_grid, (1, 0, 2, 3)), jnp.transpose(key_pad, (1, 0, 2)), jnp.transpose(value_pad, (1, 0, 2)), jnp.transpose(ctx_keys.reshape(CTX, KV_HEADS, HEAD_DIM), (1, 0, 2)), jnp.transpose(ctx_values.reshape(CTX, KV_HEADS, HEAD_DIM), (1, 0, 2)), sink.reshape(KV_HEADS, groups)))
    mixed = jnp.transpose(stacked, (1, 0, 2)).reshape(seq_total, HEADS * HEAD_DIM)
    projected = jnp.dot(mixed, w_out, preferred_element_type=jnp.float32)
    normed = projected * lax.rsqrt(lax.optimization_barrier(jnp.mean(projected * projected, axis=-1, keepdims=True)) + EPSILON) * out_gain
    return (latent.astype(jnp.float32) + gate_vec * normed).astype(jnp.bfloat16)
```

```python
import functools
import math

import jax
import jax.numpy as jnp
from jax import lax
from jax.experimental import pallas as pl
from jax.experimental.pallas import tpu as pltpu
from jax.sharding import PartitionSpec as P

HEAD_DIM = 64
WINDOW = 128
SPAN = 128
GRID_W = 64
EPSILON = 1e-06
NEG_BIG = -1e30
LANES = 128
MESH = pl.DeviceIdType.MESH
F32 = jnp.float32
BF16 = jnp.bfloat16


def dot(a, b):
    return jnp.dot(a, b, preferred_element_type=F32)


def dot_t(a, b):
    return lax.dot_general(a, b, (((1,), (1,)), ((), ())), preferred_element_type=F32)


def kernel(
    sp_n,
    tp_n,
    latent_hbm,
    cond_ref,
    ctx_hbm,
    ctx_cond_ref,
    mod_hbm,
    norm_gain_ref,
    out_gain_ref,
    wq_hbm,
    wk_hbm,
    wv_hbm,
    wo_hbm,
    sink_ref,
    out_ref,
    mod,
    ctx,
    wk,
    wv,
    latent,
    wq,
    wo,
    hidden,
    parts,
    vecs,
    rms,
    table,
    bias,
    ctx_kv,
    own_kv,
    q_rot,
    q_plain,
    mixed,
    projected,
    load_sem,
    sum_send,
    sum_recv,
    gat_send,
    gat_recv,
    z_send,
    z_recv,
    f_send,
    f_recv,
    halo_send,
    halo_recv,
):
    sp = lax.axis_index("sp")
    tp = lax.axis_index("tp")
    me = sp * tp_n + tp
    count = sp_n * tp_n
    rows, width = latent.shape
    ctx_rows = ctx.shape[0]
    key_width = wk.shape[1]
    kv_width = 2 * key_width
    piece = mod.shape[1]
    cols = mod.shape[2]
    quarter = ctx_rows // tp_n
    blocks = rows // SPAN
    pairs = key_width // LANES
    heads = wq.shape[1] // HEAD_DIM
    group = heads // (key_width // HEAD_DIM)

    barrier = pltpu.get_barrier_semaphore()
    for step in range(1, count):
        other = lax.rem(me + step, count)
        pl.semaphore_signal(
            barrier,
            inc=1,
            device_id={"sp": other // tp_n, "tp": lax.rem(other, tp_n)},
            device_id_type=MESH,
        )

    loads = []
    for at, (source, target) in enumerate(
        ((mod_hbm, mod), (ctx_hbm, ctx), (wk_hbm, wk), (wv_hbm, wv), (latent_hbm, latent), (wq_hbm, wq), (wo_hbm, wo))
    ):
        load = pltpu.make_async_copy(source, target, load_sem.at[at])
        load.start()
        loads.append(load)

    at_rows = pl.ds(pl.multiple_of(sp * piece, LANES), piece)
    own = []
    for ref in (cond_ref, ctx_cond_ref):
        v = ref[:, at_rows].astype(F32)
        own.append(jnp.broadcast_to(v / (1.0 + jnp.exp(-v)), (16, piece)))
    row_id = lax.broadcasted_iota(jnp.int32, (16, piece), 0)
    loads[0].wait()
    total = None
    for which in range(3):
        left = jnp.where(
            row_id == 2 * which, own[0], jnp.where(row_id == 2 * which + 1, own[1], 0.0)
        ).astype(BF16)
        term = dot(left, mod[which])
        total = term if total is None else total + term
    parts[sp] = total[:8]
    pl.semaphore_wait(barrier, count - 1)

    def sum_copy(step, slot):
        return pltpu.make_async_remote_copy(
            src_ref=parts.at[sp],
            dst_ref=parts.at[slot],
            send_sem=sum_send.at[step - 1],
            recv_sem=sum_recv.at[slot],
            device_id={"sp": lax.rem(sp + step, sp_n), "tp": tp},
            device_id_type=MESH,
        )

    for step in range(1, sp_n):
        sum_copy(step, sp).start()

    def row_rms(ref, at):
        x = ref[...].astype(F32)
        mean = jnp.sum(x * x, axis=-1, keepdims=True) * (1.0 / width)
        rms[at, : ref.shape[0]] = jnp.broadcast_to(lax.rsqrt(mean + EPSILON), (ref.shape[0], LANES))

    loads[1].wait()
    row_rms(ctx, 1)

    for step in range(1, sp_n):
        sum_copy(step, lax.rem(sp + step, sp_n)).wait_recv()
    summed = parts[0]
    for s in range(1, sp_n):
        summed = summed + parts[s]
    vecs[tp] = summed

    def gat_copy(step, slot):
        return pltpu.make_async_remote_copy(
            src_ref=vecs.at[tp],
            dst_ref=vecs.at[slot],
            send_sem=gat_send.at[step - 1],
            recv_sem=gat_recv.at[slot],
            device_id={"sp": sp, "tp": lax.rem(tp + step, tp_n)},
            device_id_type=MESH,
        )

    for step in range(1, tp_n):
        gat_copy(step, tp).start()

    loads[4].wait()
    row_rms(latent, 0)

    lane = lax.broadcasted_iota(jnp.int32, (rows, LANES), 1)
    low_half = (lane & (HEAD_DIM // 2)) == 0
    position = me * rows + lax.broadcasted_iota(jnp.int32, (rows, LANES), 0)
    freqs = HEAD_DIM // 4
    slot = (lane & (freqs - 1)).astype(F32)
    coord = jnp.where((lane & freqs) == 0, position // GRID_W, position % GRID_W).astype(F32)
    angle = coord * jnp.exp(slot * (-math.log(10000.0) / freqs))
    table[0] = jnp.cos(angle)
    sine = jnp.sin(angle)
    table[1] = jnp.where(low_half, -sine, sine)
    q_at = lax.broadcasted_iota(jnp.int32, (SPAN, 3 * SPAN), 0)
    k_at = lax.broadcasted_iota(jnp.int32, (SPAN, 3 * SPAN), 1) - SPAN
    for b in range(blocks):
        k_pos = me * rows + b * SPAN + k_at
        ok = (jnp.abs(q_at - k_at) <= WINDOW) & (k_pos >= 0) & (k_pos < count * rows)
        bias[b] = jnp.where(ok, 0.0, NEG_BIG)

    for step in range(1, tp_n):
        gat_copy(step, lax.rem(tp + step, tp_n)).wait_recv()

    def modulate(ref, which):
        r = rms[which, : ref.shape[0]]
        r = jnp.concatenate([r] * (cols // LANES), axis=1)
        for t in range(tp_n):
            at = pl.ds(t * cols, cols)
            gain = norm_gain_ref[:, at] * (1.0 + vecs[t, 2 + which : 3 + which])
            shift = vecs[t, which : which + 1]
            hidden[: ref.shape[0], at] = (ref[:, at].astype(F32) * r * gain + shift).astype(BF16)

    modulate(ctx, 1)
    loads[2].wait()
    loads[3].wait()
    ctx_at = pl.ds(pl.multiple_of(sp * ctx_rows, 16), ctx_rows)
    ctx_kv[ctx_at, :key_width] = dot(hidden[:ctx_rows], wk[...]).astype(BF16)
    ctx_kv[ctx_at, key_width:] = dot(hidden[:ctx_rows], wv[...]).astype(BF16)

    def share(s, t):
        return ctx_kv.at[pl.ds(pl.multiple_of(s * ctx_rows + t * quarter, 16), quarter)]

    def z_copy(step, s):
        return pltpu.make_async_remote_copy(
            src_ref=share(s, tp),
            dst_ref=share(s, tp),
            send_sem=z_send.at[step - 1],
            recv_sem=z_recv.at[s],
            device_id={"sp": lax.rem(sp + step, sp_n), "tp": tp},
            device_id_type=MESH,
        )

    def f_copy(far, step, s, t):
        return pltpu.make_async_remote_copy(
            src_ref=share(s, t),
            dst_ref=share(s, t),
            send_sem=f_send.at[(far - 1) * (tp_n - 1) + step - 1],
            recv_sem=f_recv.at[s * tp_n + t],
            device_id={"sp": sp, "tp": lax.rem(tp + step, tp_n)},
            device_id_type=MESH,
        )

    for step in range(1, sp_n):
        z_copy(step, sp).start()

    def rotate(x):
        swapped = jnp.where(
            low_half, pltpu.roll(x, LANES - HEAD_DIM // 2, 1), pltpu.roll(x, HEAD_DIM // 2, 1)
        )
        return x * table[0] + swapped * table[1]

    modulate(latent, 0)
    keys = dot(hidden[:rows], wk[...]).astype(BF16).astype(F32)
    for p in range(pairs):
        at = slice(p * LANES, (p + 1) * LANES)
        own_kv[SPAN : SPAN + rows, at] = rotate(keys[:, at]).astype(BF16)
    own_kv[SPAN : SPAN + rows, key_width:] = dot(hidden[:rows], wv[...]).astype(BF16)

    after = lax.rem(me + 1, count)
    before = lax.rem(me + count - 1, count)
    to_next = pltpu.make_async_remote_copy(
        src_ref=own_kv.at[pl.ds(rows, SPAN)],
        dst_ref=own_kv.at[pl.ds(0, SPAN)],
        send_sem=halo_send.at[0],
        recv_sem=halo_recv.at[0],
        device_id={"sp": after // tp_n, "tp": lax.rem(after, tp_n)},
        device_id_type=MESH,
    )
    to_prev = pltpu.make_async_remote_copy(
        src_ref=own_kv.at[pl.ds(SPAN, SPAN)],
        dst_ref=own_kv.at[pl.ds(SPAN + rows, SPAN)],
        send_sem=halo_send.at[1],
        recv_sem=halo_recv.at[1],
        device_id={"sp": before // tp_n, "tp": lax.rem(before, tp_n)},
        device_id_type=MESH,
    )

    @pl.when(me < count - 1)
    def _():
        to_next.start()

    @pl.when(me > 0)
    def _():
        to_prev.start()

    @pl.when(me == 0)
    def _():
        own_kv[:SPAN] = jnp.zeros((SPAN, kv_width), BF16)

    @pl.when(me == count - 1)
    def _():
        own_kv[SPAN + rows :] = jnp.zeros((SPAN, kv_width), BF16)

    in_low = lane < HEAD_DIM
    loads[5].wait()
    tile = group * HEAD_DIM
    for kv in range(heads // group):
        q = dot(hidden[:rows], wq[:, kv * tile : (kv + 1) * tile]).astype(BF16).astype(F32)
        q = q * (HEAD_DIM**-0.5)
        keep = in_low if kv % 2 == 0 else jnp.logical_not(in_low)
        for j in range(tile // LANES):
            plain = q[:, j * LANES : (j + 1) * LANES]
            for target, x in ((q_plain, plain), (q_rot, rotate(plain))):
                turned = pltpu.roll(x, HEAD_DIM, 1)
                first, second = (x, turned) if kv % 2 == 0 else (turned, x)
                h = kv * group + 2 * j
                target[h] = jnp.where(keep, first, 0.0).astype(BF16)
                target[h + 1] = jnp.where(keep, second, 0.0).astype(BF16)

    for far in range(1, sp_n):
        s = lax.rem(sp + sp_n - far, sp_n)
        z_copy(far, s).wait_recv()
        for step in range(1, tp_n):
            f_copy(far, step, s, tp).start()

    @pl.when(me > 0)
    def _():
        to_next.wait_recv()

    @pl.when(me < count - 1)
    def _():
        to_prev.wait_recv()

    for far in range(1, sp_n):
        s = lax.rem(sp + sp_n - far, sp_n)
        for step in range(1, tp_n):
            f_copy(far, step, s, lax.rem(tp + step, tp_n)).wait_recv()

    half_tiles = tile // LANES

    def attend(at, carry):
        pair = at // half_tiles
        half = lax.rem(at, half_tiles)
        k_lanes = pl.ds(pl.multiple_of(pair * LANES, LANES), LANES)
        v_lanes = pl.ds(pl.multiple_of(key_width + pair * LANES, LANES), LANES)
        k_ctx = ctx_kv[:, k_lanes]
        v_ctx = ctx_kv[:, v_lanes]
        v_ctx = jnp.concatenate([v_ctx, jnp.ones(v_ctx.shape, BF16)], axis=1)
        for parity in range(2):
            out = []
            lane_tile = (pair * 2 + parity) * half_tiles + half
            for a in range(2):
                h = lane_tile * 2 + a
                s_ctx = dot_t(q_plain[h], k_ctx)
                tops, locals_ = [], []
                for b in range(blocks):
                    s_loc = (
                        dot_t(
                            q_rot[h, b * SPAN : (b + 1) * SPAN],
                            own_kv[b * SPAN : (b + 3) * SPAN, k_lanes],
                        )
                        + bias[b]
                    )
                    locals_.append(s_loc)
                    tops.append(jnp.max(s_loc, axis=-1, keepdims=True))
                sink = sink_ref[h]
                top = jnp.maximum(
                    jnp.maximum(
                        jnp.concatenate(tops, axis=0), jnp.max(s_ctx, axis=-1, keepdims=True)
                    ),
                    sink,
                )
                acc = dot(jnp.exp(s_ctx - top).astype(BF16), v_ctx)
                near = []
                for b in range(blocks):
                    v_loc = own_kv[b * SPAN : (b + 3) * SPAN, v_lanes]
                    v_loc = jnp.concatenate([v_loc, jnp.ones(v_loc.shape, BF16)], axis=1)
                    w = jnp.exp(locals_[b] - top[b * SPAN : (b + 1) * SPAN]).astype(BF16)
                    near.append(dot(w, v_loc))
                acc = acc + jnp.concatenate(near, axis=0)
                out.append(acc[:, :LANES] / (acc[:, LANES:] + jnp.exp(sink - top)))
            if parity == 0:
                both = jnp.where(in_low, out[0], pltpu.roll(out[1], HEAD_DIM, 1))
            else:
                both = jnp.where(in_low, pltpu.roll(out[0], HEAD_DIM, 1), out[1])
            mixed[:, pl.ds(pl.multiple_of(lane_tile * LANES, LANES), LANES)] = both.astype(BF16)
        return carry

    lax.fori_loop(0, pairs * half_tiles, attend, 0)

    loads[6].wait()
    wide = 256

    def project(at, squares):
        lanes = pl.ds(pl.multiple_of(at * wide, wide), wide)
        y = dot(mixed[...], wo[:, lanes])
        projected[:, lanes] = y
        return squares + jnp.sum(y * y, axis=-1, keepdims=True)

    squares = lax.fori_loop(0, width // wide, project, jnp.zeros((rows, 1), F32))
    r = lax.rsqrt(squares * (1.0 / width) + EPSILON)
    for t in range(tp_n):
        at = pl.ds(t * cols, cols)
        gain = vecs[t, 4:5] * out_gain_ref[:, at]
        out_ref[:, at] = (latent[:, at].astype(F32) + projected[:, at] * r * gain).astype(BF16)

    for step in range(1, sp_n):
        sum_copy(step, sp).wait_send()
        z_copy(step, sp).wait_send()
    for step in range(1, tp_n):
        gat_copy(step, tp).wait_send()
        for far in range(1, sp_n):
            s = lax.rem(sp + sp_n - far, sp_n)
            f_copy(far, step, s, tp).wait_send()

    @pl.when(me < count - 1)
    def _():
        to_next.wait_send()

    @pl.when(me > 0)
    def _():
        to_prev.wait_send()


def solution(mesh):
    sp_n, tp_n = mesh.shape["sp"], mesh.shape["tp"]

    def shards(
        latent, cond, ctx_rows, ctx_cond, mod_weight, norm_gain, out_gain, w_query, w_key, w_value, w_out, sink
    ):
        rows, width = latent.shape
        context = ctx_rows.shape[0]
        key_width = w_key.shape[1]
        heads = w_query.shape[1] // HEAD_DIM
        cols = mod_weight.shape[2]
        any_spec = pl.BlockSpec(memory_space=pl.ANY)
        vmem = pl.BlockSpec(memory_space=pltpu.VMEM)
        dma = pltpu.SemaphoreType.DMA
        return pl.pallas_call(
            functools.partial(kernel, sp_n, tp_n),
            out_shape=jax.ShapeDtypeStruct((rows, width), BF16),
            in_specs=[
                any_spec,
                vmem,
                any_spec,
                vmem,
                any_spec,
                vmem,
                vmem,
                any_spec,
                any_spec,
                any_spec,
                any_spec,
                pl.BlockSpec(memory_space=pltpu.SMEM),
            ],
            out_specs=vmem,
            scratch_shapes=[
                pltpu.VMEM(mod_weight.shape, BF16),
                pltpu.VMEM(ctx_rows.shape, BF16),
                pltpu.VMEM(w_key.shape, BF16),
                pltpu.VMEM(w_value.shape, BF16),
                pltpu.VMEM(latent.shape, BF16),
                pltpu.VMEM(w_query.shape, BF16),
                pltpu.VMEM(w_out.shape, BF16),
                pltpu.VMEM((max(rows, context), width), BF16),
                pltpu.VMEM((sp_n, 8, cols), F32),
                pltpu.VMEM((tp_n, 8, cols), F32),
                pltpu.VMEM((2, max(rows, context), LANES), F32),
                pltpu.VMEM((2, rows, LANES), F32),
                pltpu.VMEM((rows // SPAN, SPAN, 3 * SPAN), F32),
                pltpu.VMEM((sp_n * context, 2 * key_width), BF16),
                pltpu.VMEM((rows + 2 * SPAN, 2 * key_width), BF16),
                pltpu.VMEM((heads, rows, LANES), BF16),
                pltpu.VMEM((heads, rows, LANES), BF16),
                pltpu.VMEM((rows, heads * HEAD_DIM), BF16),
                pltpu.VMEM((rows, width), F32),
                dma((7,)),
                dma((sp_n - 1,)),
                dma((sp_n,)),
                dma((tp_n - 1,)),
                dma((tp_n,)),
                dma((sp_n - 1,)),
                dma((sp_n,)),
                dma(((sp_n - 1) * (tp_n - 1),)),
                dma((sp_n * tp_n,)),
                dma((2,)),
                dma((2,)),
            ],
            compiler_params=pltpu.CompilerParams(
                collective_id=0, has_side_effects=True, vmem_limit_bytes=60 * 1024 * 1024
            ),
        )(
            latent,
            cond.reshape(1, -1),
            ctx_rows,
            ctx_cond.reshape(1, -1),
            mod_weight,
            norm_gain.reshape(1, -1),
            out_gain.reshape(1, -1),
            w_query,
            w_key,
            w_value,
            w_out,
            sink,
        )

    placed = (
        P(("dp", "sp", "tp"), None),
        P("dp"),
        P(("dp", "sp"), None),
        P(),
        P(None, "sp", "tp"),
        P(),
        P(),
        P(),
        P(),
        P(),
        P(),
        P(),
    )
    return jax.shard_map(
        shards, mesh=mesh, in_specs=placed, out_specs=P(("dp", "sp", "tp"), None), check_vma=False
    )
```

```python
import functools
import math

import jax
import jax.numpy as jnp
from jax import lax
from jax.experimental import pallas as pl
from jax.experimental.pallas import tpu as pltpu
from jax.sharding import PartitionSpec as P

HEAD_DIM = 64
WINDOW = 128
SPAN = 128
GRID_W = 64
EPSILON = 1e-06
NEG_BIG = -1e30
LANES = 128
MESH = pl.DeviceIdType.MESH
F32 = jnp.float32
BF16 = jnp.bfloat16


def dot(a, b):
    return jnp.dot(a, b, preferred_element_type=F32)


def dot_t(a, b):
    return lax.dot_general(a, b, (((1,), (1,)), ((), ())), preferred_element_type=F32)


def kernel(
    sp_n,
    tp_n,
    latent_hbm,
    cond_ref,
    ctx_hbm,
    ctx_cond_ref,
    mod_hbm,
    norm_gain_ref,
    out_gain_ref,
    wq_hbm,
    wk_hbm,
    wv_hbm,
    wo_hbm,
    sink_ref,
    out_ref,
    mod,
    ctx,
    wk,
    wv,
    latent,
    wq,
    wo,
    hidden,
    silu,
    parts,
    vecs,
    rms,
    table,
    bias,
    ctx_kv,
    own_kv,
    q_rot,
    q_plain,
    acc,
    tops,
    mixed,
    projected,
    load_sem,
    sum_send,
    sum_recv,
    gat_send,
    gat_recv,
    z_send,
    z_recv,
    f_send,
    f_recv,
    halo_send,
    halo_recv,
):
    sp = lax.axis_index("sp")
    tp = lax.axis_index("tp")
    me = sp * tp_n + tp
    way = 1 - 2 * ((2 * sp) // sp_n)
    count = sp_n * tp_n
    rows, width = latent.shape
    ctx_rows = ctx.shape[0]
    key_width = wk.shape[1]
    kv_width = 2 * key_width
    piece = mod.shape[1]
    cols = mod.shape[2]
    quarter = ctx_rows // tp_n
    blocks = rows // SPAN
    pairs = key_width // LANES
    heads = wq.shape[1] // HEAD_DIM
    group = heads // (key_width // HEAD_DIM)

    barrier = pltpu.get_barrier_semaphore()
    for step in range(1, count):
        other = lax.rem(me + step, count)
        pl.semaphore_signal(
            barrier,
            inc=1,
            device_id={"sp": other // tp_n, "tp": lax.rem(other, tp_n)},
            device_id_type=MESH,
        )

    loads = []
    for at, (source, target) in enumerate(
        ((mod_hbm, mod), (ctx_hbm, ctx), (wk_hbm, wk), (wv_hbm, wv), (latent_hbm, latent), (wq_hbm, wq), (wo_hbm, wo))
    ):
        load = pltpu.make_async_copy(source, target, load_sem.at[at])
        load.start()
        loads.append(load)

    own = []
    for which, ref in enumerate((cond_ref, ctx_cond_ref)):
        v = ref[...].astype(F32)
        silu[which] = v / (1.0 + jnp.exp(-v))
        tiles = [
            silu[which, pl.ds(sp * (piece // LANES) + i, 1)] for i in range(piece // LANES)
        ]
        own.append(jnp.broadcast_to(jnp.concatenate(tiles, axis=1), (16, piece)))
    row_id = lax.broadcasted_iota(jnp.int32, (16, piece), 0)
    loads[0].wait()
    total = None
    for which in range(3):
        left = jnp.where(
            row_id == 2 * which, own[0], jnp.where(row_id == 2 * which + 1, own[1], 0.0)
        ).astype(BF16)
        term = dot(left, mod[which])
        total = term if total is None else total + term
    parts[sp] = total[:8]
    pl.semaphore_wait(barrier, count - 1)

    def sum_copy(step, slot):
        return pltpu.make_async_remote_copy(
            src_ref=parts.at[sp],
            dst_ref=parts.at[slot],
            send_sem=sum_send.at[step - 1],
            recv_sem=sum_recv.at[slot],
            device_id={"sp": lax.rem(sp + step, sp_n), "tp": tp},
            device_id_type=MESH,
        )

    for step in range(1, sp_n):
        sum_copy(step, sp).start()

    def row_rms(ref, at):
        x = ref[...].astype(F32)
        mean = jnp.sum(x * x, axis=-1, keepdims=True) * (1.0 / width)
        rms[at, : ref.shape[0]] = jnp.broadcast_to(lax.rsqrt(mean + EPSILON), (ref.shape[0], LANES))

    loads[1].wait()
    row_rms(ctx, 1)

    for step in range(1, sp_n):
        sum_copy(step, lax.rem(sp + step, sp_n)).wait_recv()
    summed = parts[0]
    for s in range(1, sp_n):
        summed = summed + parts[s]
    vecs[tp] = summed

    def gat_copy(step, slot):
        return pltpu.make_async_remote_copy(
            src_ref=vecs.at[tp],
            dst_ref=vecs.at[slot],
            send_sem=gat_send.at[step - 1],
            recv_sem=gat_recv.at[slot],
            device_id={"sp": sp, "tp": lax.rem(tp + step, tp_n)},
            device_id_type=MESH,
        )

    for step in range(1, tp_n):
        gat_copy(step, tp).start()

    loads[4].wait()
    row_rms(latent, 0)

    lane = lax.broadcasted_iota(jnp.int32, (rows, LANES), 1)
    low_half = (lane & (HEAD_DIM // 2)) == 0
    position = me * rows + lax.broadcasted_iota(jnp.int32, (rows, LANES), 0)
    freqs = HEAD_DIM // 4
    slot = (lane & (freqs - 1)).astype(F32)
    coord = jnp.where((lane & freqs) == 0, position // GRID_W, position % GRID_W).astype(F32)
    angle = coord * jnp.exp(slot * (-math.log(10000.0) / freqs))
    table[0] = jnp.cos(angle)
    sine = jnp.sin(angle)
    table[1] = jnp.where(low_half, -sine, sine)
    q_at = lax.broadcasted_iota(jnp.int32, (SPAN, 3 * SPAN), 0)
    k_at = lax.broadcasted_iota(jnp.int32, (SPAN, 3 * SPAN), 1) - SPAN
    for b in range(blocks):
        k_pos = me * rows + b * SPAN + k_at
        ok = (jnp.abs(q_at - k_at) <= WINDOW) & (k_pos >= 0) & (k_pos < count * rows)
        bias[b] = jnp.where(ok, 0.0, NEG_BIG)

    for step in range(1, tp_n):
        gat_copy(step, lax.rem(tp + step, tp_n)).wait_recv()

    def modulate(ref, which):
        r = rms[which, : ref.shape[0]]
        r = jnp.concatenate([r] * (cols // LANES), axis=1)
        for t in range(tp_n):
            at = pl.ds(t * cols, cols)
            gain = norm_gain_ref[:, at] * (1.0 + vecs[t, 2 + which : 3 + which])
            shift = vecs[t, which : which + 1]
            hidden[: ref.shape[0], at] = (ref[:, at].astype(F32) * r * gain + shift).astype(BF16)

    modulate(ctx, 1)
    loads[2].wait()
    loads[3].wait()
    ctx_at = pl.ds(pl.multiple_of(sp * ctx_rows, 16), ctx_rows)
    ctx_kv[ctx_at, :key_width] = dot(hidden[:ctx_rows], wk[...]).astype(BF16)
    ctx_kv[ctx_at, key_width:] = dot(hidden[:ctx_rows], wv[...]).astype(BF16)

    def peer(step):
        return lax.rem(sp + way * step + sp_n, sp_n)

    def share(s, t):
        return ctx_kv.at[pl.ds(pl.multiple_of(s * ctx_rows + t * quarter, 16), quarter)]

    def z_copy(step, s):
        return pltpu.make_async_remote_copy(
            src_ref=share(s, tp),
            dst_ref=share(s, tp),
            send_sem=z_send.at[step - 1],
            recv_sem=z_recv.at[s],
            device_id={"sp": peer(step), "tp": tp},
            device_id_type=MESH,
        )

    def f_copy(far, step, s, t):
        return pltpu.make_async_remote_copy(
            src_ref=share(s, t),
            dst_ref=share(s, t),
            send_sem=f_send.at[(far - 1) * (tp_n - 1) + step - 1],
            recv_sem=f_recv.at[s * tp_n + t],
            device_id={"sp": sp, "tp": lax.rem(tp + step, tp_n)},
            device_id_type=MESH,
        )

    for step in range(1, sp_n):
        z_copy(step, sp).start()

    def rotate(x):
        swapped = jnp.where(
            low_half, pltpu.roll(x, LANES - HEAD_DIM // 2, 1), pltpu.roll(x, HEAD_DIM // 2, 1)
        )
        return x * table[0] + swapped * table[1]

    modulate(latent, 0)
    keys = dot(hidden[:rows], wk[...]).astype(BF16).astype(F32)
    for p in range(pairs):
        at = slice(p * LANES, (p + 1) * LANES)
        own_kv[SPAN : SPAN + rows, at] = rotate(keys[:, at]).astype(BF16)
    own_kv[SPAN : SPAN + rows, key_width:] = dot(hidden[:rows], wv[...]).astype(BF16)

    after = lax.rem(me + 1, count)
    before = lax.rem(me + count - 1, count)
    to_next = pltpu.make_async_remote_copy(
        src_ref=own_kv.at[pl.ds(rows, SPAN)],
        dst_ref=own_kv.at[pl.ds(0, SPAN)],
        send_sem=halo_send.at[0],
        recv_sem=halo_recv.at[0],
        device_id={"sp": after // tp_n, "tp": lax.rem(after, tp_n)},
        device_id_type=MESH,
    )
    to_prev = pltpu.make_async_remote_copy(
        src_ref=own_kv.at[pl.ds(SPAN, SPAN)],
        dst_ref=own_kv.at[pl.ds(SPAN + rows, SPAN)],
        send_sem=halo_send.at[1],
        recv_sem=halo_recv.at[1],
        device_id={"sp": before // tp_n, "tp": lax.rem(before, tp_n)},
        device_id_type=MESH,
    )

    @pl.when(me < count - 1)
    def _():
        to_next.start()

    @pl.when(me > 0)
    def _():
        to_prev.start()

    @pl.when(me == 0)
    def _():
        own_kv[:SPAN] = jnp.zeros((SPAN, kv_width), BF16)

    @pl.when(me == count - 1)
    def _():
        own_kv[SPAN + rows :] = jnp.zeros((SPAN, kv_width), BF16)

    in_low = lane < HEAD_DIM
    loads[5].wait()
    tile = group * HEAD_DIM
    for kv in range(heads // group):
        q = dot(hidden[:rows], wq[:, kv * tile : (kv + 1) * tile]).astype(BF16).astype(F32)
        q = q * (HEAD_DIM**-0.5)
        keep = in_low if kv % 2 == 0 else jnp.logical_not(in_low)
        for j in range(tile // LANES):
            plain = q[:, j * LANES : (j + 1) * LANES]
            for target, x in ((q_plain, plain), (q_rot, rotate(plain))):
                turned = pltpu.roll(x, HEAD_DIM, 1)
                first, second = (x, turned) if kv % 2 == 0 else (turned, x)
                h = kv * group + 2 * j
                target[h] = jnp.where(keep, first, 0.0).astype(BF16)
                target[h + 1] = jnp.where(keep, second, 0.0).astype(BF16)

    kv_heads = heads // group
    per = -(-(sp_n - 1) // kv_heads)

    def lanes_of(kv):
        pair = kv // 2
        return (
            pl.ds(pl.multiple_of(pair * LANES, LANES), LANES),
            pl.ds(pl.multiple_of(key_width + pair * LANES, LANES), LANES),
        )

    def with_ones(v):
        return jnp.concatenate([v, jnp.ones(v.shape, BF16)], axis=1)

    def forward(far):
        s = peer(far)
        z_copy(far, s).wait_recv()
        for step in range(1, tp_n):
            f_copy(far, step, s, tp).start()

    def own_block(kv, carry):
        for i in range(per):
            far = kv * per + i + 1

            @pl.when(far < sp_n)
            def _():
                forward(far)

        k_lanes, v_lanes = lanes_of(kv)
        k = ctx_kv[ctx_at, k_lanes]
        v = with_ones(ctx_kv[ctx_at, v_lanes])
        for g in range(group):
            h = kv * group + g
            scores = dot_t(q_plain[h], k)
            sink = sink_ref[h]
            top = jnp.maximum(jnp.max(scores, axis=-1, keepdims=True), sink)
            weights = jnp.exp(scores - top).astype(BF16)
            term = dot(weights, v)
            acc[h, :, :LANES] = term[:, :LANES]
            acc[h, :, LANES:] = term[:, LANES:] + jnp.exp(sink - top)
            tops[h] = jnp.broadcast_to(top, (rows, LANES))
        return carry

    lax.fori_loop(0, kv_heads, own_block, 0)

    def update(h, at, old, top, term):
        decay = jnp.exp(old - top)
        acc[h, at, :LANES] = acc[h, at, :LANES] * decay + term[:, :LANES]
        acc[h, at, LANES:] = acc[h, at, LANES:] * decay + term[:, LANES:]
        tops[h, at] = top

    @pl.when(me > 0)
    def _():
        to_next.wait_recv()

    @pl.when(me < count - 1)
    def _():
        to_prev.wait_recv()

    def window(kv, carry):
        k_lanes, v_lanes = lanes_of(kv)
        for b in range(blocks):
            at = pl.ds(b * SPAN, SPAN)
            band = pl.ds(b * SPAN, 3 * SPAN)
            k = own_kv[band, k_lanes]
            v = with_ones(own_kv[band, v_lanes])
            for g in range(group):
                h = kv * group + g
                scores = dot_t(q_rot[h, at], k) + bias[b]
                old = tops[h, at]
                top = jnp.maximum(old, jnp.max(scores, axis=-1, keepdims=True))
                weights = jnp.exp(scores - jnp.concatenate([top] * 3, axis=1)).astype(BF16)
                update(h, at, old, top, dot(weights, v))
        return carry

    lax.fori_loop(0, kv_heads, window, 0)

    def far_block(far, carry):
        s = peer(far)
        for step in range(1, tp_n):
            f_copy(far, step, s, lax.rem(tp + step, tp_n)).wait_recv()
        block = pl.ds(pl.multiple_of(s * ctx_rows, 16), ctx_rows)

        def one(kv, inner):
            k_lanes, v_lanes = lanes_of(kv)
            k = ctx_kv[block, k_lanes]
            v = with_ones(ctx_kv[block, v_lanes])
            for g in range(group):
                h = kv * group + g
                scores = dot_t(q_plain[h], k)
                old = tops[h]
                top = jnp.maximum(old, jnp.max(scores, axis=-1, keepdims=True))
                weights = jnp.exp(scores - top[:, :1]).astype(BF16)
                update(h, pl.ds(0, rows), old, top, dot(weights, v))
            return inner

        return lax.fori_loop(0, kv_heads, one, carry)

    lax.fori_loop(1, sp_n, far_block, 0)

    half_tiles = tile // LANES
    for lane_tile in range(heads // 2):
        out = []
        for h in (2 * lane_tile, 2 * lane_tile + 1):
            out.append(acc[h, :, :LANES] / acc[h, :, LANES:])
        if (lane_tile // half_tiles) % 2 == 0:
            both = jnp.where(in_low, out[0], pltpu.roll(out[1], HEAD_DIM, 1))
        else:
            both = jnp.where(in_low, pltpu.roll(out[0], HEAD_DIM, 1), out[1])
        mixed[:, lane_tile * LANES : (lane_tile + 1) * LANES] = both.astype(BF16)

    loads[6].wait()
    wide = 256

    def project(at, squares):
        lanes = pl.ds(pl.multiple_of(at * wide, wide), wide)
        y = dot(mixed[...], wo[:, lanes])
        projected[:, lanes] = y
        return squares + jnp.sum(y * y, axis=-1, keepdims=True)

    squares = lax.fori_loop(0, width // wide, project, jnp.zeros((rows, 1), F32))
    r = lax.rsqrt(squares * (1.0 / width) + EPSILON)
    for t in range(tp_n):
        at = pl.ds(t * cols, cols)
        gain = vecs[t, 4:5] * out_gain_ref[:, at]
        out_ref[:, at] = (latent[:, at].astype(F32) + projected[:, at] * r * gain).astype(BF16)

    for step in range(1, sp_n):
        sum_copy(step, sp).wait_send()
        z_copy(step, sp).wait_send()
    for step in range(1, tp_n):
        gat_copy(step, tp).wait_send()
        for far in range(1, sp_n):
            s = peer(far)
            f_copy(far, step, s, tp).wait_send()

    @pl.when(me < count - 1)
    def _():
        to_next.wait_send()

    @pl.when(me > 0)
    def _():
        to_prev.wait_send()


def solution(mesh):
    sp_n, tp_n = mesh.shape["sp"], mesh.shape["tp"]

    def shards(
        latent, cond, ctx_rows, ctx_cond, mod_weight, norm_gain, out_gain, w_query, w_key, w_value, w_out, sink
    ):
        rows, width = latent.shape
        context = ctx_rows.shape[0]
        key_width = w_key.shape[1]
        heads = w_query.shape[1] // HEAD_DIM
        cols = mod_weight.shape[2]
        any_spec = pl.BlockSpec(memory_space=pl.ANY)
        vmem = pl.BlockSpec(memory_space=pltpu.VMEM)
        dma = pltpu.SemaphoreType.DMA
        return pl.pallas_call(
            functools.partial(kernel, sp_n, tp_n),
            out_shape=jax.ShapeDtypeStruct((rows, width), BF16),
            in_specs=[
                any_spec,
                vmem,
                any_spec,
                vmem,
                any_spec,
                vmem,
                vmem,
                any_spec,
                any_spec,
                any_spec,
                any_spec,
                pl.BlockSpec(memory_space=pltpu.SMEM),
            ],
            out_specs=vmem,
            scratch_shapes=[
                pltpu.VMEM(mod_weight.shape, BF16),
                pltpu.VMEM(ctx_rows.shape, BF16),
                pltpu.VMEM(w_key.shape, BF16),
                pltpu.VMEM(w_value.shape, BF16),
                pltpu.VMEM(latent.shape, BF16),
                pltpu.VMEM(w_query.shape, BF16),
                pltpu.VMEM(w_out.shape, BF16),
                pltpu.VMEM((max(rows, context), width), BF16),
                pltpu.VMEM((2, width // LANES, LANES), F32),
                pltpu.VMEM((sp_n, 8, cols), F32),
                pltpu.VMEM((tp_n, 8, cols), F32),
                pltpu.VMEM((2, max(rows, context), LANES), F32),
                pltpu.VMEM((2, rows, LANES), F32),
                pltpu.VMEM((rows // SPAN, SPAN, 3 * SPAN), F32),
                pltpu.VMEM((sp_n * context, 2 * key_width), BF16),
                pltpu.VMEM((rows + 2 * SPAN, 2 * key_width), BF16),
                pltpu.VMEM((heads, rows, LANES), BF16),
                pltpu.VMEM((heads, rows, LANES), BF16),
                pltpu.VMEM((heads, rows, 2 * LANES), F32),
                pltpu.VMEM((heads, rows, LANES), F32),
                pltpu.VMEM((rows, heads * HEAD_DIM), BF16),
                pltpu.VMEM((rows, width), F32),
                dma((7,)),
                dma((sp_n - 1,)),
                dma((sp_n,)),
                dma((tp_n - 1,)),
                dma((tp_n,)),
                dma((sp_n - 1,)),
                dma((sp_n,)),
                dma(((sp_n - 1) * (tp_n - 1),)),
                dma((sp_n * tp_n,)),
                dma((2,)),
                dma((2,)),
            ],
            compiler_params=pltpu.CompilerParams(
                collective_id=0, has_side_effects=True, vmem_limit_bytes=60 * 1024 * 1024
            ),
        )(
            latent,
            cond.reshape(-1, LANES),
            ctx_rows,
            ctx_cond.reshape(-1, LANES),
            mod_weight,
            norm_gain.reshape(1, -1),
            out_gain.reshape(1, -1),
            w_query,
            w_key,
            w_value,
            w_out,
            sink,
        )

    placed = (
        P(("dp", "sp", "tp"), None),
        P("dp"),
        P(("dp", "sp"), None),
        P(),
        P(None, "sp", "tp"),
        P(),
        P(),
        P(),
        P(),
        P(),
        P(),
        P(),
    )
    return jax.shard_map(
        shards, mesh=mesh, in_specs=placed, out_specs=P(("dp", "sp", "tp"), None), check_vma=False
    )
```

```python
import functools
import math

import jax
import jax.numpy as jnp
from jax import lax
from jax.experimental import pallas as pl
from jax.experimental.pallas import tpu as pltpu
from jax.sharding import PartitionSpec as P

HEAD_DIM = 64
WINDOW = 128
SPAN = 128
GRID_W = 64
EPSILON = 1e-06
NEG_BIG = -1e30
LANES = 128
MESH = pl.DeviceIdType.MESH
F32 = jnp.float32
BF16 = jnp.bfloat16


def dot(a, b):
    return jnp.dot(a, b, preferred_element_type=F32)


def dot_t(a, b):
    return lax.dot_general(a, b, (((1,), (1,)), ((), ())), preferred_element_type=F32)


def kernel(
    sp_n,
    tp_n,
    latent_hbm,
    cond_ref,
    ctx_hbm,
    ctx_cond_ref,
    mod_hbm,
    norm_gain_ref,
    out_gain_ref,
    wq_hbm,
    wk_hbm,
    wv_hbm,
    wo_hbm,
    sink_ref,
    out_ref,
    mod,
    ctx,
    wk,
    wv,
    latent,
    wq,
    wo,
    hidden,
    silu,
    parts,
    vecs,
    rms,
    table,
    bias,
    ctx_kv,
    own_kv,
    q_rot,
    q_plain,
    acc,
    tops,
    mixed,
    projected,
    load_sem,
    sum_send,
    sum_recv,
    gat_send,
    gat_recv,
    z_send,
    z_recv,
    f_send,
    f_recv,
    halo_send,
    halo_recv,
):
    sp = lax.axis_index("sp")
    tp = lax.axis_index("tp")
    me = sp * tp_n + tp
    way = 1 - 2 * ((2 * sp) // sp_n)
    count = sp_n * tp_n
    rows, width = latent.shape
    ctx_rows = ctx.shape[0]
    key_width = wk.shape[1]
    kv_width = 2 * key_width
    piece = mod.shape[1]
    cols = mod.shape[2]
    quarter = ctx_rows // tp_n
    blocks = rows // SPAN
    pairs = key_width // LANES
    heads = wq.shape[1] // HEAD_DIM
    group = heads // (key_width // HEAD_DIM)

    loads = []
    for at, (source, target) in enumerate(
        ((mod_hbm, mod), (ctx_hbm, ctx), (wk_hbm, wk), (wv_hbm, wv), (latent_hbm, latent), (wq_hbm, wq), (wo_hbm, wo))
    ):
        loads.append(pltpu.make_async_copy(source, target, load_sem.at[at]))
    loads[0].start()

    barrier = pltpu.get_barrier_semaphore()
    for step in range(1, count):
        other = lax.rem(me + step, count)
        pl.semaphore_signal(
            barrier,
            inc=1,
            device_id={"sp": other // tp_n, "tp": lax.rem(other, tp_n)},
            device_id_type=MESH,
        )

    own = []
    for which, ref in enumerate((cond_ref, ctx_cond_ref)):
        v = ref[...].astype(F32)
        silu[which] = v / (1.0 + jnp.exp(-v))
        tiles = [
            silu[which, pl.ds(sp * (piece // LANES) + i, 1)] for i in range(piece // LANES)
        ]
        own.append(jnp.broadcast_to(jnp.concatenate(tiles, axis=1), (16, piece)))
    row_id = lax.broadcasted_iota(jnp.int32, (16, piece), 0)
    loads[0].wait()
    for at in (1, 2, 3, 4):
        loads[at].start()
    total = None
    for which in range(3):
        left = jnp.where(
            row_id == 2 * which, own[0], jnp.where(row_id == 2 * which + 1, own[1], 0.0)
        ).astype(BF16)
        term = dot(left, mod[which])
        total = term if total is None else total + term
    parts[sp] = total[:8]
    pl.semaphore_wait(barrier, count - 1)

    def sum_copy(step, slot):
        return pltpu.make_async_remote_copy(
            src_ref=parts.at[sp],
            dst_ref=parts.at[slot],
            send_sem=sum_send.at[step - 1],
            recv_sem=sum_recv.at[slot],
            device_id={"sp": lax.rem(sp + step, sp_n), "tp": tp},
            device_id_type=MESH,
        )

    for step in range(1, sp_n):
        sum_copy(step, sp).start()

    def row_rms(ref, at):
        x = ref[...].astype(F32)
        mean = jnp.sum(x * x, axis=-1, keepdims=True) * (1.0 / width)
        rms[at, : ref.shape[0]] = jnp.broadcast_to(lax.rsqrt(mean + EPSILON), (ref.shape[0], LANES))

    loads[1].wait()
    loads[5].start()
    row_rms(ctx, 1)

    for step in range(1, sp_n):
        sum_copy(step, lax.rem(sp + step, sp_n)).wait_recv()
    summed = parts[0]
    for s in range(1, sp_n):
        summed = summed + parts[s]
    vecs[tp] = summed

    def gat_copy(step, slot):
        return pltpu.make_async_remote_copy(
            src_ref=vecs.at[tp],
            dst_ref=vecs.at[slot],
            send_sem=gat_send.at[step - 1],
            recv_sem=gat_recv.at[slot],
            device_id={"sp": sp, "tp": lax.rem(tp + step, tp_n)},
            device_id_type=MESH,
        )

    for step in range(1, tp_n):
        gat_copy(step, tp).start()

    loads[4].wait()
    row_rms(latent, 0)
    loads[6].start()

    lane = lax.broadcasted_iota(jnp.int32, (rows, LANES), 1)
    low_half = (lane & (HEAD_DIM // 2)) == 0
    position = me * rows + lax.broadcasted_iota(jnp.int32, (rows, LANES), 0)
    freqs = HEAD_DIM // 4
    slot = (lane & (freqs - 1)).astype(F32)
    coord = jnp.where((lane & freqs) == 0, position // GRID_W, position % GRID_W).astype(F32)
    angle = coord * jnp.exp(slot * (-math.log(10000.0) / freqs))
    table[0] = jnp.cos(angle)
    sine = jnp.sin(angle)
    table[1] = jnp.where(low_half, -sine, sine)
    q_at = lax.broadcasted_iota(jnp.int32, (SPAN, 3 * SPAN), 0)
    k_at = lax.broadcasted_iota(jnp.int32, (SPAN, 3 * SPAN), 1) - SPAN
    for b in range(blocks):
        k_pos = me * rows + b * SPAN + k_at
        ok = (jnp.abs(q_at - k_at) <= WINDOW) & (k_pos >= 0) & (k_pos < count * rows)
        bias[b] = jnp.where(ok, 0.0, NEG_BIG)

    for step in range(1, tp_n):
        gat_copy(step, lax.rem(tp + step, tp_n)).wait_recv()

    def modulate(ref, which):
        r = rms[which, : ref.shape[0]]
        r = jnp.concatenate([r] * (cols // LANES), axis=1)
        for t in range(tp_n):
            at = pl.ds(t * cols, cols)
            gain = norm_gain_ref[:, at] * (1.0 + vecs[t, 2 + which : 3 + which])
            shift = vecs[t, which : which + 1]
            hidden[: ref.shape[0], at] = (ref[:, at].astype(F32) * r * gain + shift).astype(BF16)

    modulate(ctx, 1)
    loads[2].wait()
    loads[3].wait()
    ctx_at = pl.ds(pl.multiple_of(sp * ctx_rows, 16), ctx_rows)
    ctx_kv[ctx_at, :key_width] = dot(hidden[:ctx_rows], wk[...]).astype(BF16)
    ctx_kv[ctx_at, key_width:] = dot(hidden[:ctx_rows], wv[...]).astype(BF16)

    def peer(step):
        return lax.rem(sp + way * step + sp_n, sp_n)

    def share(s, t):
        return ctx_kv.at[pl.ds(pl.multiple_of(s * ctx_rows + t * quarter, 16), quarter)]

    def z_copy(step, s):
        return pltpu.make_async_remote_copy(
            src_ref=share(s, tp),
            dst_ref=share(s, tp),
            send_sem=z_send.at[step - 1],
            recv_sem=z_recv.at[s],
            device_id={"sp": peer(step), "tp": tp},
            device_id_type=MESH,
        )

    def f_copy(far, step, s, t):
        return pltpu.make_async_remote_copy(
            src_ref=share(s, t),
            dst_ref=share(s, t),
            send_sem=f_send.at[(far - 1) * (tp_n - 1) + step - 1],
            recv_sem=f_recv.at[s * tp_n + t],
            device_id={"sp": sp, "tp": lax.rem(tp + step, tp_n)},
            device_id_type=MESH,
        )

    for step in range(1, sp_n):
        z_copy(step, sp).start()

    def rotate(x):
        swapped = jnp.where(
            low_half, pltpu.roll(x, LANES - HEAD_DIM // 2, 1), pltpu.roll(x, HEAD_DIM // 2, 1)
        )
        return x * table[0] + swapped * table[1]

    modulate(latent, 0)
    keys = dot(hidden[:rows], wk[...]).astype(BF16).astype(F32)
    for p in range(pairs):
        at = slice(p * LANES, (p + 1) * LANES)
        own_kv[SPAN : SPAN + rows, at] = rotate(keys[:, at]).astype(BF16)
    own_kv[SPAN : SPAN + rows, key_width:] = dot(hidden[:rows], wv[...]).astype(BF16)

    after = lax.rem(me + 1, count)
    before = lax.rem(me + count - 1, count)
    to_next = pltpu.make_async_remote_copy(
        src_ref=own_kv.at[pl.ds(rows, SPAN)],
        dst_ref=own_kv.at[pl.ds(0, SPAN)],
        send_sem=halo_send.at[0],
        recv_sem=halo_recv.at[0],
        device_id={"sp": after // tp_n, "tp": lax.rem(after, tp_n)},
        device_id_type=MESH,
    )
    to_prev = pltpu.make_async_remote_copy(
        src_ref=own_kv.at[pl.ds(SPAN, SPAN)],
        dst_ref=own_kv.at[pl.ds(SPAN + rows, SPAN)],
        send_sem=halo_send.at[1],
        recv_sem=halo_recv.at[1],
        device_id={"sp": before // tp_n, "tp": lax.rem(before, tp_n)},
        device_id_type=MESH,
    )

    @pl.when(me < count - 1)
    def _():
        to_next.start()

    @pl.when(me > 0)
    def _():
        to_prev.start()

    @pl.when(me == 0)
    def _():
        own_kv[:SPAN] = jnp.zeros((SPAN, kv_width), BF16)

    @pl.when(me == count - 1)
    def _():
        own_kv[SPAN + rows :] = jnp.zeros((SPAN, kv_width), BF16)

    in_low = lane < HEAD_DIM
    loads[5].wait()
    tile = group * HEAD_DIM
    for kv in range(heads // group):
        q = dot(hidden[:rows], wq[:, kv * tile : (kv + 1) * tile]).astype(BF16).astype(F32)
        q = q * (HEAD_DIM**-0.5)
        keep = in_low if kv % 2 == 0 else jnp.logical_not(in_low)
        for j in range(tile // LANES):
            plain = q[:, j * LANES : (j + 1) * LANES]
            for target, x in ((q_plain, plain), (q_rot, rotate(plain))):
                turned = pltpu.roll(x, HEAD_DIM, 1)
                first, second = (x, turned) if kv % 2 == 0 else (turned, x)
                h = kv * group + 2 * j
                target[h] = jnp.where(keep, first, 0.0).astype(BF16)
                target[h + 1] = jnp.where(keep, second, 0.0).astype(BF16)

    kv_heads = heads // group
    per = -(-(sp_n - 1) // kv_heads)

    def lanes_of(kv):
        pair = kv // 2
        return (
            pl.ds(pl.multiple_of(pair * LANES, LANES), LANES),
            pl.ds(pl.multiple_of(key_width + pair * LANES, LANES), LANES),
        )

    def with_ones(v):
        return jnp.concatenate([v, jnp.ones(v.shape, BF16)], axis=1)

    def forward(far):
        s = peer(far)
        z_copy(far, s).wait_recv()
        for step in range(1, tp_n):
            f_copy(far, step, s, tp).start()

    def own_block(kv, carry):
        for i in range(per):
            far = kv * per + i + 1

            @pl.when(far < sp_n)
            def _():
                forward(far)

        k_lanes, v_lanes = lanes_of(kv)
        k = ctx_kv[ctx_at, k_lanes]
        v = with_ones(ctx_kv[ctx_at, v_lanes])
        for g in range(group):
            h = kv * group + g
            scores = dot_t(q_plain[h], k)
            sink = sink_ref[h]
            top = jnp.maximum(jnp.max(scores, axis=-1, keepdims=True), sink)
            weights = jnp.exp(scores - top).astype(BF16)
            term = dot(weights, v)
            acc[h, :, :LANES] = term[:, :LANES]
            acc[h, :, LANES:] = term[:, LANES:] + jnp.exp(sink - top)
            tops[h] = jnp.broadcast_to(top, (rows, LANES))
        return carry

    lax.fori_loop(0, kv_heads, own_block, 0)

    def update(h, at, old, top, term):
        decay = jnp.exp(old - top)
        acc[h, at, :LANES] = acc[h, at, :LANES] * decay + term[:, :LANES]
        acc[h, at, LANES:] = acc[h, at, LANES:] * decay + term[:, LANES:]
        tops[h, at] = top

    @pl.when(me > 0)
    def _():
        to_next.wait_recv()

    @pl.when(me < count - 1)
    def _():
        to_prev.wait_recv()

    def window(kv, carry):
        k_lanes, v_lanes = lanes_of(kv)
        for b in range(blocks):
            at = pl.ds(b * SPAN, SPAN)
            band = pl.ds(b * SPAN, 3 * SPAN)
            k = own_kv[band, k_lanes]
            v = with_ones(own_kv[band, v_lanes])
            for g in range(group):
                h = kv * group + g
                scores = dot_t(q_rot[h, at], k) + bias[b]
                old = tops[h, at]
                top = jnp.maximum(old, jnp.max(scores, axis=-1, keepdims=True))
                weights = jnp.exp(scores - jnp.concatenate([top] * 3, axis=1)).astype(BF16)
                update(h, at, old, top, dot(weights, v))
        return carry

    lax.fori_loop(0, kv_heads, window, 0)

    def far_block(far, carry):
        s = peer(far)
        for step in range(1, tp_n):
            f_copy(far, step, s, lax.rem(tp + step, tp_n)).wait_recv()
        block = pl.ds(pl.multiple_of(s * ctx_rows, 16), ctx_rows)

        def one(kv, inner):
            k_lanes, v_lanes = lanes_of(kv)
            k = ctx_kv[block, k_lanes]
            v = with_ones(ctx_kv[block, v_lanes])
            for g in range(group):
                h = kv * group + g
                scores = dot_t(q_plain[h], k)
                old = tops[h]
                top = jnp.maximum(old, jnp.max(scores, axis=-1, keepdims=True))
                weights = jnp.exp(scores - top[:, :1]).astype(BF16)
                update(h, pl.ds(0, rows), old, top, dot(weights, v))
            return inner

        return lax.fori_loop(0, kv_heads, one, carry)

    lax.fori_loop(1, sp_n, far_block, 0)

    half_tiles = tile // LANES
    for lane_tile in range(heads // 2):
        out = []
        for h in (2 * lane_tile, 2 * lane_tile + 1):
            out.append(acc[h, :, :LANES] / acc[h, :, LANES:])
        if (lane_tile // half_tiles) % 2 == 0:
            both = jnp.where(in_low, out[0], pltpu.roll(out[1], HEAD_DIM, 1))
        else:
            both = jnp.where(in_low, pltpu.roll(out[0], HEAD_DIM, 1), out[1])
        mixed[:, lane_tile * LANES : (lane_tile + 1) * LANES] = both.astype(BF16)

    loads[6].wait()
    wide = 256

    def project(at, squares):
        lanes = pl.ds(pl.multiple_of(at * wide, wide), wide)
        y = dot(mixed[...], wo[:, lanes])
        projected[:, lanes] = y
        return squares + jnp.sum(y * y, axis=-1, keepdims=True)

    squares = lax.fori_loop(0, width // wide, project, jnp.zeros((rows, 1), F32))
    r = lax.rsqrt(squares * (1.0 / width) + EPSILON)
    for t in range(tp_n):
        at = pl.ds(t * cols, cols)
        gain = vecs[t, 4:5] * out_gain_ref[:, at]
        out_ref[:, at] = (latent[:, at].astype(F32) + projected[:, at] * r * gain).astype(BF16)

    for step in range(1, sp_n):
        sum_copy(step, sp).wait_send()
        z_copy(step, sp).wait_send()
    for step in range(1, tp_n):
        gat_copy(step, tp).wait_send()
        for far in range(1, sp_n):
            s = peer(far)
            f_copy(far, step, s, tp).wait_send()

    @pl.when(me < count - 1)
    def _():
        to_next.wait_send()

    @pl.when(me > 0)
    def _():
        to_prev.wait_send()


def solution(mesh):
    sp_n, tp_n = mesh.shape["sp"], mesh.shape["tp"]

    def shards(
        latent, cond, ctx_rows, ctx_cond, mod_weight, norm_gain, out_gain, w_query, w_key, w_value, w_out, sink
    ):
        rows, width = latent.shape
        context = ctx_rows.shape[0]
        key_width = w_key.shape[1]
        heads = w_query.shape[1] // HEAD_DIM
        cols = mod_weight.shape[2]
        any_spec = pl.BlockSpec(memory_space=pl.ANY)
        vmem = pl.BlockSpec(memory_space=pltpu.VMEM)
        dma = pltpu.SemaphoreType.DMA
        return pl.pallas_call(
            functools.partial(kernel, sp_n, tp_n),
            out_shape=jax.ShapeDtypeStruct((rows, width), BF16),
            in_specs=[
                any_spec,
                vmem,
                any_spec,
                vmem,
                any_spec,
                vmem,
                vmem,
                any_spec,
                any_spec,
                any_spec,
                any_spec,
                pl.BlockSpec(memory_space=pltpu.SMEM),
            ],
            out_specs=vmem,
            scratch_shapes=[
                pltpu.VMEM(mod_weight.shape, BF16),
                pltpu.VMEM(ctx_rows.shape, BF16),
                pltpu.VMEM(w_key.shape, BF16),
                pltpu.VMEM(w_value.shape, BF16),
                pltpu.VMEM(latent.shape, BF16),
                pltpu.VMEM(w_query.shape, BF16),
                pltpu.VMEM(w_out.shape, BF16),
                pltpu.VMEM((max(rows, context), width), BF16),
                pltpu.VMEM((2, width // LANES, LANES), F32),
                pltpu.VMEM((sp_n, 8, cols), F32),
                pltpu.VMEM((tp_n, 8, cols), F32),
                pltpu.VMEM((2, max(rows, context), LANES), F32),
                pltpu.VMEM((2, rows, LANES), F32),
                pltpu.VMEM((rows // SPAN, SPAN, 3 * SPAN), F32),
                pltpu.VMEM((sp_n * context, 2 * key_width), BF16),
                pltpu.VMEM((rows + 2 * SPAN, 2 * key_width), BF16),
                pltpu.VMEM((heads, rows, LANES), BF16),
                pltpu.VMEM((heads, rows, LANES), BF16),
                pltpu.VMEM((heads, rows, 2 * LANES), F32),
                pltpu.VMEM((heads, rows, LANES), F32),
                pltpu.VMEM((rows, heads * HEAD_DIM), BF16),
                pltpu.VMEM((rows, width), F32),
                dma((7,)),
                dma((sp_n - 1,)),
                dma((sp_n,)),
                dma((tp_n - 1,)),
                dma((tp_n,)),
                dma((sp_n - 1,)),
                dma((sp_n,)),
                dma(((sp_n - 1) * (tp_n - 1),)),
                dma((sp_n * tp_n,)),
                dma((2,)),
                dma((2,)),
            ],
            compiler_params=pltpu.CompilerParams(
                collective_id=0, has_side_effects=True, vmem_limit_bytes=60 * 1024 * 1024
            ),
        )(
            latent,
            cond.reshape(-1, LANES),
            ctx_rows,
            ctx_cond.reshape(-1, LANES),
            mod_weight,
            norm_gain.reshape(1, -1),
            out_gain.reshape(1, -1),
            w_query,
            w_key,
            w_value,
            w_out,
            sink,
        )

    placed = (
        P(("dp", "sp", "tp"), None),
        P("dp"),
        P(("dp", "sp"), None),
        P(),
        P(None, "sp", "tp"),
        P(),
        P(),
        P(),
        P(),
        P(),
        P(),
        P(),
    )
    return jax.shard_map(
        shards, mesh=mesh, in_specs=placed, out_specs=P(("dp", "sp", "tp"), None), check_vma=False
    )
```
